32 devices in a mesh: grp: 2 (over x), ep: 16 (over z, y, core).
Axes of the slice: x: 2, y: 2, z: 4, core: 2. Of those that a mesh axis runs over, the one named last changes fastest.
Arguments:
- tokens: bfloat16 [8192, 2048], P(('grp', 'ep')), parts along dimension 0, may hold values from -6 to 6
- norm_gain: float32 [2048], replicated, may hold values from 0.1 to 1.9
- route_ids: int32 [8192, 2], P(('grp', 'ep')), parts along dimension 0, may hold values from 0 to 15, as said below
- route_slots: int32 [8192, 2], P(('grp', 'ep')), parts along dimension 0, may hold values from 0 to 47, as said below
- route_weights: float32 [8192, 2], P(('grp', 'ep')), parts along dimension 0, may hold values from 0.1 to 1
- w_gate: bfloat16 [16, 2048, 512], P('ep'), may hold values from -0.125 to 0.125
- w_up: bfloat16 [16, 2048, 512], P('ep'), may hold values from -0.125 to 0.125
- w_down: bfloat16 [16, 512, 2048], P('ep'), may hold values from -0.25 to 0.25
Outputs:
- expert_mix: bfloat16 [8192, 2048], P(('grp', 'ep')), parts along dimension 0
The draws below stay inside these ranges and needn't reach their ends.
There are 2 independent parts, one for each index of `grp`. The reference program is written for one: setup_inputs(seed, part) draws one part's arguments, and reference() takes and returns one part's arrays. A program takes and returns all parts, laid end to end along the dimension named above; an argument that names none is the same for every part. Nothing has to cross between parts.
Inputs may be any that keep to these rules, and one draw needn't show every extreme that they name: `route_ids`: expert e belongs to group e // 4. Each token names 2 different experts of one group. In each aligned block of 256 tokens (the rows of one device) no expert is named more than 48 times, and some expert exactly 48 times. `route_slots`: in each aligned block of 256 tokens, the entries that name one expert hold distinct slots 0, 1, ... up to their count less one.
All inputs are finite; a program needn't handle non-finite values.
Results may differ from the reference program's by a relative error of at most 0.007.
Values may be sent and summed in bfloat16 or wider, within the bound.
A program may use at most 64 MiB of HBM per device.

```python
import math
import jax
import jax.numpy as jnp
from jax import lax

D = 2048
FE = 512
TOPK = 2
TOK_DEV = 256
EXPERTS = 16
CAP = 48
TOKENS = 4096


def route_table(key):
    n_blocks = TOKENS // TOK_DEV
    per_group = EXPERTS // 4
    busy_count = CAP * per_group // 2
    rest_count = TOK_DEV - busy_count
    block_keys = jax.random.split(jax.random.fold_in(key, 7), n_blocks)

    def one_block(block_key):
        key_busy, key_first, key_second, key_perm, key_base, key_shift = jax.random.split(block_key, 6)
        busy = jax.random.randint(key_busy, (), 0, 4)
        low_first = jnp.maximum(0, rest_count - 2 * busy_count)
        high_first = jnp.minimum(busy_count, rest_count)
        count_first = jax.random.randint(key_first, (), low_first, high_first + 1)
        low_second = jnp.maximum(0, rest_count - count_first - busy_count)
        high_second = jnp.minimum(busy_count, rest_count - count_first)
        count_second = jax.random.randint(key_second, (), low_second, high_second + 1)
        others = jnp.stack([count_first, count_second, rest_count - count_first - count_second]).astype(jnp.int32)
        group_ids = jnp.arange(4, dtype=jnp.int32)
        other_idx = jnp.clip(group_ids - (group_ids > busy).astype(jnp.int32), 0, 2)
        counts = jnp.where(group_ids == busy, busy_count, others[other_idx]).astype(jnp.int32)
        ends = jnp.cumsum(counts)
        starts = ends - counts
        places = jnp.arange(TOK_DEV, dtype=jnp.int32)
        group_sorted = jnp.sum((places[:, None] >= ends[None, :3]).astype(jnp.int32), axis=1)
        rank_sorted = places - starts[group_sorted]
        perm = jax.random.permutation(key_perm, TOK_DEV)
        group_tok = jnp.zeros((TOK_DEV,), jnp.int32).at[perm].set(group_sorted)
        rank_tok = jnp.zeros((TOK_DEV,), jnp.int32).at[perm].set(rank_sorted)
        base = jax.random.randint(key_base, (4,), 0, per_group)
        shift = jax.random.randint(key_shift, (4,), 1, per_group)
        first = group_tok * per_group + (base[group_tok] + rank_tok) % per_group
        second = group_tok * per_group + (base[group_tok] + rank_tok + shift[group_tok]) % per_group
        ids = jnp.stack([first, second], axis=1).astype(jnp.int32)
        flat_ids = ids.reshape(-1)
        onehot = (flat_ids[:, None] == jnp.arange(EXPERTS, dtype=jnp.int32)[None, :]).astype(jnp.int32)
        slots = jnp.sum(jnp.cumsum(onehot, axis=0) * onehot, axis=1) - 1
        return (ids, slots.reshape(TOK_DEV, 2).astype(jnp.int32))
    ids, slots = jax.vmap(one_block)(block_keys)
    return (ids.reshape(TOKENS, 2), slots.reshape(TOKENS, 2))


def draw_route_ids(key, part):
    return route_table(key)[0]


def draw_route_slots(key, part):
    return route_table(key)[1]


def block_levels(rng, extent, shards, low, largest):
    loudness, own = 1.0, jax.random.fold_in(rng, 6)
    for dim, shards_of in shards:
        heights = jnp.exp(jax.random.uniform(jax.random.fold_in(own, dim), (shards_of,), jnp.float32, low / len(shards), largest / len(shards)))
        loudness = loudness * jnp.repeat(heights, extent[dim] // shards_of).reshape([-1 if axis == dim else 1 for axis in range(len(extent))])
    return loudness


def scatter_about(key, dims, spread, reach, cuts=(), kind=jnp.bfloat16):
    drawn = spread * jax.random.normal(key, dims, jnp.float32)
    if cuts:
        drawn = drawn * block_levels(key, dims, cuts, -0.22, 0.18)
    return jnp.clip(drawn, -reach, reach).astype(kind)


def setup_inputs(seed: int = 0, part: int = 0) -> dict:
    streams_of = jax.random.split(jax.random.key(seed), 9)
    own_keys = jax.random.split(jax.random.fold_in(streams_of[8], part), 9)
    return {
        "tokens": scatter_about(own_keys[0], (TOKENS, D), 1.0, 6.0, ((0, 16),)),
        "norm_gain": jnp.clip(1.0 + 0.18 * jax.random.normal(streams_of[1], (D,), jnp.float32), 0.1, 1.9),
        "route_ids": draw_route_ids(jax.random.fold_in(jax.random.fold_in(streams_of[8], part), 71), part),
        "route_slots": draw_route_slots(jax.random.fold_in(jax.random.fold_in(streams_of[8], part), 71), part),
        "route_weights": jnp.clip(jnp.exp(math.log(1.0) - 2.3025851 * jax.random.uniform(own_keys[4], (TOKENS, TOPK), jnp.float32) ** block_levels(own_keys[4], (TOKENS, TOPK), ((0, 16),), -0.2, 0.2)), 0.1, 1.0),
        "w_gate": scatter_about(streams_of[5], (EXPERTS, D, FE), D ** -0.5, 0.125, ((0, 16),)),
        "w_up": scatter_about(streams_of[6], (EXPERTS, D, FE), D ** -0.5, 0.125, ((0, 16),)),
        "w_down": scatter_about(streams_of[7], (EXPERTS, FE, D), FE ** -0.5, 0.25, ((0, 16),)),
    }


def reference(tokens, norm_gain, route_ids, route_slots, route_weights, w_gate, w_up, w_down):
    tok_f32 = tokens.astype(jnp.float32)
    scale = lax.rsqrt(lax.optimization_barrier(jnp.mean(tok_f32 * tok_f32, axis=-1, keepdims=True)) + 1e-06)
    normed = (tok_f32 * scale * norm_gain.astype(jnp.float32)).astype(jnp.bfloat16)
    n_blocks = TOKENS // TOK_DEV
    block_of = (jnp.arange(TOKENS, dtype=jnp.int32) // TOK_DEV).astype(jnp.int32)
    place_idx = (route_ids * (n_blocks * CAP) + block_of[:, None] * CAP + route_slots).astype(jnp.int32)
    buffer = jnp.zeros((EXPERTS * n_blocks * CAP, D), jnp.bfloat16)
    buffer = buffer.at[place_idx.reshape(-1)].set(jnp.repeat(normed, TOPK, axis=0))
    buffer = buffer.reshape(EXPERTS, n_blocks * CAP, D)

    def expert_apply(args):
        rows_in, gate_w, up_w, down_w = args
        gate_act = jnp.dot(rows_in, gate_w, preferred_element_type=jnp.float32)
        up_act = jnp.dot(rows_in, up_w, preferred_element_type=jnp.float32)
        hidden = (jax.nn.silu(gate_act) * up_act).astype(jnp.bfloat16)
        return jnp.dot(hidden, down_w, preferred_element_type=jnp.float32).astype(jnp.bfloat16)
    results = lax.map(expert_apply, (buffer, w_gate, w_up, w_down))
    flat_rows = results.reshape(EXPERTS * n_blocks * CAP, D)
    picked = flat_rows[place_idx].astype(jnp.float32)
    mixed = lax.optimization_barrier(jnp.sum(route_weights[:, :, None] * picked, axis=1))
    return mixed.astype(jnp.bfloat16)
```

```python
import functools

import jax
import jax.numpy as jnp
from jax import lax
from jax.experimental import pallas as pl
from jax.experimental.pallas import tpu as pltpu
from jax.sharding import PartitionSpec as P

GROUPS = 4
FACTS = 16
LANES = 128
CHUNKS = 4
SCHEDULE = (
    "D10", "U00", "D11", "U01", "D12", "D20", "U02", "D13", "C0", "D21", "U10", "U11", "D22", "U12", "D23", "R00",
    "C1", "U20", "U21", "U22", "C2", "D30", "M20", "D31", "M21", "M22", "R10", "R11", "D32", "M23", "D33", "R12",
    "U30", "U31", "U32", "C3", "R13", "R01", "R02", "R03", "M30", "M31", "M32", "M33", "M10", "M11", "M12", "M13",
    "F0", "F1", "F2", "F3",
)
NT = (((1,), (1,)), ((), ()))
F32 = jnp.float32
BF16 = jnp.bfloat16


def flip(index, bits):
    out, weight = index, 1
    while weight <= bits:
        if bits & weight:
            out = out + weight * (1 - 2 * ((index // weight) % 2))
        weight *= 2
    return out


def where01(hit):
    return jnp.where(hit, 1.0, 0.0).astype(BF16)


def iota(shape, dim):
    return lax.broadcasted_iota(jnp.int32, shape, dim)


def dot(a, b):
    return jnp.dot(a, b, preferred_element_type=F32)


def dot_nt(a, b):
    return lax.dot_general(a, b, NT, preferred_element_type=F32)


def kernel(
    peers, capp,
    tok_hbm, gain_hbm, ids_hbm, slots_hbm, wts_hbm, wg_hbm, wu_hbm, wd_hbm,
    out,
    tok, gain, ids, slots, wts, wg, wu, wd,
    normed, chosen, n_out, n_in, about, spreads, picks, own_picks, homes, home_w,
    x_out, x_in, y_out, e_in, acc, hid, r_out, r_in, m_out, h_in,
    l_sem, w_sem, ns, nr, xs, xr, ys, yr, rs, rr, hs, hr,
):
    rows, feat = tok.shape
    ffn = wg.shape[1]
    block, width = x_out.shape[2:]
    spread = peers * capp
    me = lax.axis_index("ep")
    group, rank = me // peers, me % peers
    inner = (group % 2 + group // 2) % 2
    shift = peers.bit_length() - 1
    mesh_id = pl.DeviceIdType.MESH

    def at(d, j):
        return {"ep": flip(group, d) * peers + flip(rank, j)}

    order = [0, 2 - inner, 1 + inner, 3]

    barrier = pltpu.get_barrier_semaphore()
    for d in range(1, GROUPS):
        pl.semaphore_signal(barrier, inc=1, device_id=at(d, 0), device_id_type=mesh_id)
    for j in range(1, peers):
        pl.semaphore_signal(barrier, inc=1, device_id=at(0, j), device_id_type=mesh_id)

    def fetch(pairs, sem):
        copies = [pltpu.make_async_copy(src, dst, sem.at[i]) for i, (src, dst) in enumerate(pairs)]
        for copy in copies:
            copy.start()
        return copies

    small = fetch(
        ((ids_hbm, ids), (slots_hbm, slots), (wts_hbm, wts), (gain_hbm, gain), (tok_hbm, tok)), l_sem
    )

    def send(src, dst, sent, got, where):
        pltpu.make_async_remote_copy(
            src_ref=src, dst_ref=dst, send_sem=sent, recv_sem=got,
            device_id=where, device_id_type=mesh_id,
        ).start()

    def receive(dst, got):
        pltpu.make_async_remote_copy(
            src_ref=dst, dst_ref=dst, send_sem=xs.at[0], recv_sem=got,
            device_id=at(1, 0), device_id_type=mesh_id,
        ).wait_recv()

    for copy in small[:3]:
        copy.wait()
    tok_group = ids[0:1, :] >> shift
    member = where01(iota((16, rows), 0) == tok_group)
    before = dot(member, where01(iota((rows, rows), 0) < iota((rows, rows), 1)))
    place = jnp.sum(before * member.astype(F32), axis=0, keepdims=True)
    kind = iota((FACTS, rows), 0)
    facts = jnp.where(kind == 8, tok_group.astype(F32), jnp.where(kind == 9, place, 0.0))
    codes = []
    for k in range(2):
        code = ((ids[k:k + 1, :] & (peers - 1)) ^ rank) * capp + slots[k:k + 1, :] + 1
        codes.append(code)
        facts = jnp.where(kind == k, code.astype(F32), facts)
        w = wts[k:k + 1, :]
        for part in range(3):
            piece = w.astype(BF16).astype(F32)
            facts = jnp.where(kind == 2 + 3 * k + part, piece, facts)
            w = w - piece
    facts = facts.astype(BF16)
    slot = iota((spread, rows), 0) + 1
    chosen[:spread, :] = where01(((slot == codes[0]) | (slot == codes[1])) & (tok_group == group))
    row_no = iota((block, rows), 0).astype(F32)
    n_out[...] = jnp.zeros_like(n_out)
    for d in range(1, GROUPS):
        mine = where01((row_no == place) & (tok_group == flip(group, d)))
        chosen[spread + (d - 1) * block:spread + d * block, :] = mine
        n_out[d - 1, :, :block] = dot_nt(facts, mine).astype(BF16)

    for copy in small[3:]:
        copy.wait()
    loads = fetch(((wg_hbm, wg), (wu_hbm, wu), (wd_hbm, wd)), w_sem)
    step = 32

    def norm_rows(i, carry):
        at_rows = pl.ds(pl.multiple_of(i * step, step), step)
        v = tok[at_rows, :].astype(F32)
        scale = lax.rsqrt(jnp.mean(v * v, axis=-1, keepdims=True) + 1e-06)
        normed[at_rows, :] = (v * scale * gain[...]).astype(BF16)
        return carry

    lax.fori_loop(0, rows // step, norm_rows, 0, unroll=True)

    far_first = list(range(2, peers)) + [1]
    theirs = pl.ds(capp, spread - capp)

    def send_spread(s, c):
        d = order[s]
        for j in far_first:
            send(y_out.at[d, c, pl.ds((j - 1) * capp, capp)], e_in.at[d, c, pl.ds(j * capp, capp)],
                 ys.at[0], yr.at[d, c], at(0, j))

    def send_back(d, c):
        for j in far_first:
            send(r_out.at[d, c, pl.ds((j - 1) * capp, capp)], r_in.at[d, c, pl.ds(j * capp, capp)],
                 rs.at[0], rr.at[d, c], at(0, j))

    def send_group(d, c):
        send(x_out.at[d - 1, c], x_in.at[d - 1, c], xs.at[0], xr.at[d - 1, c], at(d, 0))

    for c in range(CHUNKS):
        got = dot(chosen[...], normed[:, c * width:(c + 1) * width]).astype(BF16)
        e_in[0, c, :capp, :] = got[:capp]
        y_out[0, c, :, :] = got[capp:spread]
        for d in range(1, GROUPS):
            x_out[d - 1, c, :, :] = got[spread + (d - 1) * block:spread + d * block]
        if c == 0:
            pl.semaphore_wait(barrier, GROUPS - 1 + peers - 1)
            for d in range(1, GROUPS):
                send(n_out.at[d - 1], n_in.at[d - 1], ns.at[0], nr.at[d - 1], at(d, 0))
        send_spread(0, c)
        send_group(1, c)
        if c == 0:
            send_group(2, c)
    for c in range(1, CHUNKS):
        send_group(2, c)
    for c in range(CHUNKS):
        send_group(3, c)

    columns = dot_nt(where01(iota((rows, rows), 0) == iota((rows, rows), 1)), facts)
    slot = (iota((rows, spread), 1) + 1).astype(F32)
    ours = columns[:, 8:9] == group.astype(F32)
    for k in range(2):
        own_picks[k] = where01((slot == columns[:, k:k + 1]) & ours)
        b = 2 + 3 * k
        home_w[k] = columns[:, b:b + 1] + columns[:, b + 1:b + 2] + columns[:, b + 2:b + 3]
    slot = iota((rows, block), 1).astype(F32)
    for d in range(1, GROUPS):
        homes[d - 1] = where01((slot == columns[:, 9:10]) & (columns[:, 8:9] == flip(group, d).astype(F32)))

    def dispatch(s, c):
        d = order[s]
        if c == 0:
            receive(n_in.at[d - 1], nr.at[d - 1])
            info = n_in[d - 1]
            code = info[:, :block].astype(F32)
            slot = (iota((spread, block), 0) + 1).astype(F32)
            spreads[d - 1] = where01((slot == code[0:1, :]) | (slot == code[1:2, :]))
        receive(x_in.at[d - 1, c], xr.at[d - 1, c])
        got = dot(spreads[d - 1], x_in[d - 1, c]).astype(BF16)
        e_in[d, c, :capp, :] = got[:capp]
        y_out[d, c, :, :] = got[capp:]
        send_spread(s, c)
        if c == CHUNKS - 1:
            info = n_in[d - 1]
            facts_of = dot_nt(where01(iota((block, LANES), 0) == iota((block, LANES), 1)), info)
            about[d - 1] = facts_of
            slot = (iota((block, spread), 1) + 1).astype(F32)
            for k in range(2):
                picks[d - 1, k] = where01(slot == facts_of[:, k:k + 1])

    half = min(256, ffn)

    def partial(s, c, w, f):
        return dot(e_in[order[s], c], w[c * width:(c + 1) * width, f])

    def gather(s, c):
        d = order[s]
        if loads:
            for load in loads:
                load.wait()
            loads.clear()
        receive(e_in.at[d, c, theirs], yr.at[d, c])
        if c < CHUNKS - 1:
            for i, w in enumerate((wg, wu)):
                for f in range(0, ffn, half):
                    f = slice(f, f + half)
                    if c == 0:
                        acc[d, i, :, f] = partial(s, c, w, f)
                    else:
                        acc[d, i, :, f] += partial(s, c, w, f)

    def compute(s):
        d, c = order[s], CHUNKS - 1
        gather(s, c)
        for f in range(0, ffn, half):
            f = slice(f, f + half)
            gate = acc[d, 0, :, f] + partial(s, c, wg, f)
            upper = acc[d, 1, :, f] + partial(s, c, wu, f)
            hid[:, f] = (gate / (1.0 + jnp.exp(-gate)) * upper).astype(BF16)
        for c in range(CHUNKS):
            got = dot(hid[...], wd[:, c * width:(c + 1) * width]).astype(BF16)
            r_in[d, c, :capp, :] = got[:capp]
            r_out[d, c, :, :] = got[capp:]
            if s > 1:
                send_back(s, c)

    def mix(d, c):
        facts_of = about[d - 1]
        weigh = [facts_of[:, b:b + 1] + facts_of[:, b + 1:b + 2] + facts_of[:, b + 2:b + 3] for b in (2, 5)]
        receive(r_in.at[d, c, theirs], rr.at[d, c])
        got = r_in[d, c]
        mixed = weigh[0] * dot(picks[d - 1, 0], got) + weigh[1] * dot(picks[d - 1, 1], got)
        m_out[d - 1, c, :, :] = mixed.astype(BF16)
        send(m_out.at[d - 1, c], h_in.at[d - 1, c], hs.at[0], hr.at[d - 1, c], at(d, 0))

    def finish(c):
        receive(r_in.at[0, c, theirs], rr.at[0, c])
        got = r_in[0, c]
        total = home_w[0] * dot(own_picks[0], got) + home_w[1] * dot(own_picks[1], got)
        for d in range(1, GROUPS):
            receive(h_in.at[d - 1, c], hr.at[d - 1, c])
        total += sum(dot(homes[d - 1], h_in[d - 1, c]) for d in range(1, GROUPS))
        out[:, c * width:(c + 1) * width] = total.astype(BF16)

    stages = {"D": dispatch, "U": gather, "C": compute, "R": send_back, "M": mix, "F": finish}
    for item in SCHEDULE:
        stages[item[0]](*(int(i) for i in item[1:]))

    for src, dst, sent, got in (
        (n_out, n_in, ns, nr), (x_out, x_in, xs, xr), (y_out, r_out, ys, yr), (r_out, y_out, rs, rr), (m_out, h_in, hs, hr),
    ):
        pltpu.make_async_remote_copy(
            src_ref=src, dst_ref=dst, send_sem=sent.at[0], recv_sem=got.at[(0,) * len(got.shape)],
            device_id=at(1, 0), device_id_type=mesh_id,
        ).wait_send()


def shards(tokens, norm_gain, route_ids, route_slots, route_weights, w_gate, w_up, w_down):
    rows, feat = tokens.shape
    n_devices = lax.axis_size("ep")
    top_count = route_ids.shape[1]
    cap = 3 * top_count * rows // (2 * n_devices)
    capp = -(-cap // 16) * 16
    peers = n_devices // GROUPS
    block = peers * cap // top_count
    spread = peers * capp
    ffn = w_gate.shape[2]
    width = feat // CHUNKS
    others = GROUPS - 1
    anywhere = pl.BlockSpec(memory_space=pl.ANY)
    vmem = pl.BlockSpec(memory_space=pltpu.VMEM)
    dma = pltpu.SemaphoreType.DMA

    def buf(*shape, kind=BF16):
        return pltpu.VMEM(shape, kind)

    return pl.pallas_call(
        functools.partial(kernel, peers, capp),
        out_shape=pltpu.VMEM((rows, feat), BF16),
        in_specs=[anywhere] * 8,
        out_specs=vmem,
        scratch_shapes=[
            buf(rows, feat), buf(1, feat, kind=F32), buf(top_count, rows, kind=jnp.int32),
            buf(top_count, rows, kind=jnp.int32), buf(top_count, rows, kind=F32),
            buf(feat, ffn), buf(feat, ffn), buf(ffn, feat),
            buf(rows, feat), buf(spread + others * block, rows),
            buf(others, FACTS, LANES), buf(others, FACTS, LANES), buf(others, block, FACTS, kind=F32),
            buf(others, spread, block), buf(others, 2, block, spread), buf(2, rows, spread),
            buf(others, rows, block), buf(2, rows, 1, kind=F32),
            buf(others, CHUNKS, block, width), buf(others, CHUNKS, block, width),
            buf(GROUPS, CHUNKS, spread - capp, width), buf(GROUPS, CHUNKS, spread, width),
            buf(GROUPS, 2, spread, ffn, kind=F32), buf(spread, ffn),
            buf(GROUPS, CHUNKS, spread - capp, width), buf(GROUPS, CHUNKS, spread, width),
            buf(others, CHUNKS, block, width), buf(others, CHUNKS, block, width),
            dma((5,)), dma((3,)),
            dma((1,)), dma((others,)),
            dma((1,)), dma((others, CHUNKS)),
            dma((1,)), dma((GROUPS, CHUNKS)),
            dma((1,)), dma((GROUPS, CHUNKS)),
            dma((1,)), dma((others, CHUNKS)),
        ],
        compiler_params=pltpu.CompilerParams(
            collective_id=0, has_side_effects=True, vmem_limit_bytes=60 * 1024 * 1024
        ),
    )(
        tokens, norm_gain.reshape(1, feat), route_ids.T, route_slots.T, route_weights.T,
        w_gate.reshape(feat, ffn), w_up.reshape(feat, ffn), w_down.reshape(ffn, feat),
    )


def solution(mesh):
    placed = (
        P(("grp", "ep"), None),
        P(),
        P(("grp", "ep"), None),
        P(("grp", "ep"), None),
        P(("grp", "ep"), None),
        P("ep", None, None),
        P("ep", None, None),
        P("ep", None, None),
    )
    return jax.shard_map(
        shards, mesh=mesh, in_specs=placed, out_specs=P(("grp", "ep"), None), check_vma=False
    )
```

```python
import functools

import jax
import jax.numpy as jnp
from jax import lax
from jax.experimental import pallas as pl
from jax.experimental.pallas import tpu as pltpu
from jax.sharding import PartitionSpec as P

GROUPS = 4
FACTS = 16
LANES = 128
CHUNKS = 4
SCHEDULE = (
    "D10", "U00", "D11", "U01", "D12", "X", "D20", "U02", "D13", "C0", "D21", "U10", "U11", "D22", "U12", "D23",
    "R00", "C1", "U20", "U21", "U22", "C2", "D30", "M20", "D31", "M21", "D32", "M22", "M23", "D33", "R10", "U30",
    "U31", "U32", "C3", "R11", "R12", "R13", "R01", "R02", "R03", "M10", "M30", "M31", "M32", "M33", "M11", "M12",
    "M13", "F0", "F1", "F2", "F3",
)
NT = (((1,), (1,)), ((), ()))
F32 = jnp.float32
BF16 = jnp.bfloat16


def flip(index, bits):
    out, weight = index, 1
    while weight <= bits:
        if bits & weight:
            out = out + weight * (1 - 2 * ((index // weight) % 2))
        weight *= 2
    return out


def where01(hit):
    return jnp.where(hit, 1.0, 0.0).astype(BF16)


def iota(shape, dim):
    return lax.broadcasted_iota(jnp.int32, shape, dim)


def dot(a, b):
    return jnp.dot(a, b, preferred_element_type=F32)


def dot_nt(a, b):
    return lax.dot_general(a, b, NT, preferred_element_type=F32)


def kernel(
    peers, capp,
    tok_hbm, gain_hbm, ids_hbm, slots_hbm, wts_hbm, wg_hbm, wu_hbm, wd_hbm,
    out,
    tok, gain, ids, slots, wts, wg, wu, wd,
    normed, chosen, n_out, n_in, about, spreads, picks, own_picks, homes, home_w,
    x_out, x_in, y_out, e_in, acc, hid, r_out, r_in, m_out, h_in,
    l_sem, w_sem, ns, nr, xs, xr, ys, yr, rs, rr, hs, hr,
):
    rows, feat = tok.shape
    ffn = wg.shape[1]
    block, width = x_out.shape[2:]
    spread = peers * capp
    me = lax.axis_index("ep")
    group, rank = me // peers, me % peers
    inner = (group % 2 + group // 2) % 2
    shift = peers.bit_length() - 1
    mesh_id = pl.DeviceIdType.MESH

    def at(d, j):
        return {"ep": flip(group, d) * peers + flip(rank, j)}

    order = [0, 2 - inner, 1 + inner, 3]

    barrier = pltpu.get_barrier_semaphore()
    for d in range(1, GROUPS):
        pl.semaphore_signal(barrier, inc=1, device_id=at(d, 0), device_id_type=mesh_id)
    for j in range(1, peers):
        pl.semaphore_signal(barrier, inc=1, device_id=at(0, j), device_id_type=mesh_id)

    def fetch(pairs, sem):
        copies = [pltpu.make_async_copy(src, dst, sem.at[i]) for i, (src, dst) in enumerate(pairs)]
        for copy in copies:
            copy.start()
        return copies

    small = fetch(
        ((ids_hbm, ids), (slots_hbm, slots), (wts_hbm, wts), (gain_hbm, gain), (tok_hbm, tok)), l_sem
    )

    def send(src, dst, sent, got, where):
        pltpu.make_async_remote_copy(
            src_ref=src, dst_ref=dst, send_sem=sent, recv_sem=got,
            device_id=where, device_id_type=mesh_id,
        ).start()

    def receive(dst, got):
        pltpu.make_async_remote_copy(
            src_ref=dst, dst_ref=dst, send_sem=xs.at[0], recv_sem=got,
            device_id=at(1, 0), device_id_type=mesh_id,
        ).wait_recv()

    for copy in small[:3]:
        copy.wait()
    tok_group = ids[0:1, :] >> shift
    member = where01(iota((16, rows), 0) == tok_group)
    before = dot(member, where01(iota((rows, rows), 0) < iota((rows, rows), 1)))
    place = jnp.sum(before * member.astype(F32), axis=0, keepdims=True)
    kind = iota((FACTS, rows), 0)
    facts = jnp.where(kind == 8, tok_group.astype(F32), jnp.where(kind == 9, place, 0.0))
    codes = []
    for k in range(2):
        code = ((ids[k:k + 1, :] & (peers - 1)) ^ rank) * capp + slots[k:k + 1, :] + 1
        codes.append(code)
        facts = jnp.where(kind == k, code.astype(F32), facts)
        w = wts[k:k + 1, :]
        for part in range(3):
            piece = w.astype(BF16).astype(F32)
            facts = jnp.where(kind == 2 + 3 * k + part, piece, facts)
            w = w - piece
    facts = facts.astype(BF16)
    slot = iota((spread, rows), 0) + 1
    chosen[:spread, :] = where01(((slot == codes[0]) | (slot == codes[1])) & (tok_group == group))
    row_no = iota((block, rows), 0).astype(F32)
    n_out[...] = jnp.zeros_like(n_out)
    for d in range(1, GROUPS):
        mine = where01((row_no == place) & (tok_group == flip(group, d)))
        chosen[spread + (d - 1) * block:spread + d * block, :] = mine
        n_out[d - 1, :, :block] = dot_nt(facts, mine).astype(BF16)

    for copy in small[3:]:
        copy.wait()
    loads = fetch(((wg_hbm, wg), (wu_hbm, wu), (wd_hbm, wd)), w_sem)
    step = 32

    def norm_rows(i, carry):
        at_rows = pl.ds(pl.multiple_of(i * step, step), step)
        v = tok[at_rows, :].astype(F32)
        scale = lax.rsqrt(jnp.mean(v * v, axis=-1, keepdims=True) + 1e-06)
        normed[at_rows, :] = (v * scale * gain[...]).astype(BF16)
        return carry

    lax.fori_loop(0, rows // step, norm_rows, 0, unroll=True)

    far_first = list(range(2, peers)) + [1]
    theirs = pl.ds(capp, spread - capp)

    def send_spread(s, c):
        d = order[s]
        for j in far_first:
            send(y_out.at[d, c, pl.ds((j - 1) * capp, capp)], e_in.at[d, c, pl.ds(j * capp, capp)],
                 ys.at[0], yr.at[d, c], at(0, j))

    def send_back(d, c):
        for j in far_first:
            send(r_out.at[d, c, pl.ds((j - 1) * capp, capp)], r_in.at[d, c, pl.ds(j * capp, capp)],
                 rs.at[0], rr.at[d, c], at(0, j))

    def send_group(d, c):
        send(x_out.at[d - 1, c], x_in.at[d - 1, c], xs.at[0], xr.at[d - 1, c], at(d, 0))

    for c in range(CHUNKS):
        got = dot(chosen[...], normed[:, c * width:(c + 1) * width]).astype(BF16)
        e_in[0, c, :capp, :] = got[:capp]
        y_out[0, c, :, :] = got[capp:spread]
        for d in range(1, GROUPS):
            x_out[d - 1, c, :, :] = got[spread + (d - 1) * block:spread + d * block]
        if c == 0:
            pl.semaphore_wait(barrier, GROUPS - 1 + peers - 1)
            for d in range(1, GROUPS):
                send(n_out.at[d - 1], n_in.at[d - 1], ns.at[0], nr.at[d - 1], at(d, 0))
        send_spread(0, c)
        send_group(1, c)

        @pl.when(inner == 1)
        def _():
            send_group(2, c)

    columns = dot_nt(where01(iota((rows, rows), 0) == iota((rows, rows), 1)), facts)
    slot = (iota((rows, spread), 1) + 1).astype(F32)
    ours = columns[:, 8:9] == group.astype(F32)
    for k in range(2):
        own_picks[k] = where01((slot == columns[:, k:k + 1]) & ours)
        b = 2 + 3 * k
        home_w[k] = columns[:, b:b + 1] + columns[:, b + 1:b + 2] + columns[:, b + 2:b + 3]
    slot = iota((rows, block), 1).astype(F32)
    for d in range(1, GROUPS):
        homes[d - 1] = where01((slot == columns[:, 9:10]) & (columns[:, 8:9] == flip(group, d).astype(F32)))

    def dispatch(s, c):
        d = order[s]
        if c == 0:
            receive(n_in.at[d - 1], nr.at[d - 1])
            info = n_in[d - 1]
            code = info[:, :block].astype(F32)
            slot = (iota((spread, block), 0) + 1).astype(F32)
            spreads[d - 1] = where01((slot == code[0:1, :]) | (slot == code[1:2, :]))
        receive(x_in.at[d - 1, c], xr.at[d - 1, c])
        got = dot(spreads[d - 1], x_in[d - 1, c]).astype(BF16)
        e_in[d, c, :capp, :] = got[:capp]
        y_out[d, c, :, :] = got[capp:]
        send_spread(s, c)
        if c == CHUNKS - 1:
            info = n_in[d - 1]
            facts_of = dot_nt(where01(iota((block, LANES), 0) == iota((block, LANES), 1)), info)
            about[d - 1] = facts_of
            slot = (iota((block, spread), 1) + 1).astype(F32)
            for k in range(2):
                picks[d - 1, k] = where01(slot == facts_of[:, k:k + 1])

    def send_far():
        @pl.when(inner == 0)
        def _():
            for c in range(CHUNKS):
                send_group(2, c)

        for c in range(CHUNKS):
            send_group(3, c)

    half = min(256, ffn)

    def partial(s, c, w, f):
        return dot(e_in[order[s], c], w[c * width:(c + 1) * width, f])

    def gather(s, c):
        d = order[s]
        if loads:
            for load in loads:
                load.wait()
            loads.clear()
        receive(e_in.at[d, c, theirs], yr.at[d, c])
        if c < CHUNKS - 1:
            for i, w in enumerate((wg, wu)):
                for f in range(0, ffn, half):
                    f = slice(f, f + half)
                    if c == 0:
                        acc[d, i, :, f] = partial(s, c, w, f)
                    else:
                        acc[d, i, :, f] += partial(s, c, w, f)

    def compute(s):
        d, c = order[s], CHUNKS - 1
        gather(s, c)
        for f in range(0, ffn, half):
            f = slice(f, f + half)
            gate = acc[d, 0, :, f] + partial(s, c, wg, f)
            upper = acc[d, 1, :, f] + partial(s, c, wu, f)
            hid[:, f] = (gate / (1.0 + jnp.exp(-gate)) * upper).astype(BF16)
        for c in range(CHUNKS):
            got = dot(hid[...], wd[:, c * width:(c + 1) * width]).astype(BF16)
            r_in[d, c, :capp, :] = got[:capp]
            r_out[d, c, :, :] = got[capp:]
            if s > 1:
                send_back(s, c)

    def mix(d, c):
        facts_of = about[d - 1]
        weigh = [facts_of[:, b:b + 1] + facts_of[:, b + 1:b + 2] + facts_of[:, b + 2:b + 3] for b in (2, 5)]
        receive(r_in.at[d, c, theirs], rr.at[d, c])
        got = r_in[d, c]
        mixed = weigh[0] * dot(picks[d - 1, 0], got) + weigh[1] * dot(picks[d - 1, 1], got)
        m_out[d - 1, c, :, :] = mixed.astype(BF16)
        send(m_out.at[d - 1, c], h_in.at[d - 1, c], hs.at[0], hr.at[d - 1, c], at(d, 0))

    def finish(c):
        receive(r_in.at[0, c, theirs], rr.at[0, c])
        got = r_in[0, c]
        total = home_w[0] * dot(own_picks[0], got) + home_w[1] * dot(own_picks[1], got)
        for d in range(1, GROUPS):
            receive(h_in.at[d - 1, c], hr.at[d - 1, c])
        total += sum(dot(homes[d - 1], h_in[d - 1, c]) for d in range(1, GROUPS))
        out[:, c * width:(c + 1) * width] = total.astype(BF16)

    stages = {"X": send_far, "D": dispatch, "U": gather, "C": compute, "R": send_back, "M": mix, "F": finish}
    for item in SCHEDULE:
        stages[item[0]](*(int(i) for i in item[1:]))

    for src, dst, sent, got in (
        (n_out, n_in, ns, nr), (x_out, x_in, xs, xr), (y_out, r_out, ys, yr), (r_out, y_out, rs, rr), (m_out, h_in, hs, hr),
    ):
        pltpu.make_async_remote_copy(
            src_ref=src, dst_ref=dst, send_sem=sent.at[0], recv_sem=got.at[(0,) * len(got.shape)],
            device_id=at(1, 0), device_id_type=mesh_id,
        ).wait_send()


def shards(tokens, norm_gain, route_ids, route_slots, route_weights, w_gate, w_up, w_down):
    rows, feat = tokens.shape
    n_devices = lax.axis_size("ep")
    top_count = route_ids.shape[1]
    cap = 3 * top_count * rows // (2 * n_devices)
    capp = -(-cap // 16) * 16
    peers = n_devices // GROUPS
    block = peers * cap // top_count
    spread = peers * capp
    ffn = w_gate.shape[2]
    width = feat // CHUNKS
    others = GROUPS - 1
    anywhere = pl.BlockSpec(memory_space=pl.ANY)
    vmem = pl.BlockSpec(memory_space=pltpu.VMEM)
    dma = pltpu.SemaphoreType.DMA

    def buf(*shape, kind=BF16):
        return pltpu.VMEM(shape, kind)

    return pl.pallas_call(
        functools.partial(kernel, peers, capp),
        out_shape=pltpu.VMEM((rows, feat), BF16),
        in_specs=[anywhere] * 8,
        out_specs=vmem,
        scratch_shapes=[
            buf(rows, feat), buf(1, feat, kind=F32), buf(top_count, rows, kind=jnp.int32),
            buf(top_count, rows, kind=jnp.int32), buf(top_count, rows, kind=F32),
            buf(feat, ffn), buf(feat, ffn), buf(ffn, feat),
            buf(rows, feat), buf(spread + others * block, rows),
            buf(others, FACTS, LANES), buf(others, FACTS, LANES), buf(others, block, FACTS, kind=F32),
            buf(others, spread, block), buf(others, 2, block, spread), buf(2, rows, spread),
            buf(others, rows, block), buf(2, rows, 1, kind=F32),
            buf(others, CHUNKS, block, width), buf(others, CHUNKS, block, width),
            buf(GROUPS, CHUNKS, spread - capp, width), buf(GROUPS, CHUNKS, spread, width),
            buf(GROUPS, 2, spread, ffn, kind=F32), buf(spread, ffn),
            buf(GROUPS, CHUNKS, spread - capp, width), buf(GROUPS, CHUNKS, spread, width),
            buf(others, CHUNKS, block, width), buf(others, CHUNKS, block, width),
            dma((5,)), dma((3,)),
            dma((1,)), dma((others,)),
            dma((1,)), dma((others, CHUNKS)),
            dma((1,)), dma((GROUPS, CHUNKS)),
            dma((1,)), dma((GROUPS, CHUNKS)),
            dma((1,)), dma((others, CHUNKS)),
        ],
        compiler_params=pltpu.CompilerParams(
            collective_id=0, has_side_effects=True, vmem_limit_bytes=60 * 1024 * 1024
        ),
    )(
        tokens, norm_gain.reshape(1, feat), route_ids.T, route_slots.T, route_weights.T,
        w_gate.reshape(feat, ffn), w_up.reshape(feat, ffn), w_down.reshape(ffn, feat),
    )


def solution(mesh):
    placed = (
        P(("grp", "ep"), None),
        P(),
        P(("grp", "ep"), None),
        P(("grp", "ep"), None),
        P(("grp", "ep"), None),
        P("ep", None, None),
        P("ep", None, None),
        P("ep", None, None),
    )
    return jax.shard_map(
        shards, mesh=mesh, in_specs=placed, out_specs=P(("grp", "ep"), None), check_vma=False
    )
```

```python
import functools

import jax
import jax.numpy as jnp
from jax import lax
from jax.experimental import pallas as pl
from jax.experimental.pallas import tpu as pltpu
from jax.sharding import PartitionSpec as P

GROUPS = 4
FACTS = 16
LANES = 128
CHUNKS = 4
HELD = 2
NEAR_FIRST = 2
SCHEDULE = (
    "D10", "U00", "D11", "U01", "D12", "X", "D20", "U02", "D13", "C0", "D21", "U10", "U11", "D22", "U12", "D23",
    "Q000", "C1", "Q110", "U20", "U21", "U22", "C2", "D30", "M20", "D31", "M21", "D32", "M22", "N", "D33", "M23",
    "Q010", "B0", "U30", "U31", "U32", "C3", "B1", "Q100", "R01", "R02", "R03", "L0", "L1", "L2", "L3", "L4",
    "L5", "L6", "L7", "F0", "F1", "F2", "F3",
)
NT = (((1,), (1,)), ((), ()))
F32 = jnp.float32
BF16 = jnp.bfloat16


def flip(index, bits):
    out, weight = index, 1
    while weight <= bits:
        if bits & weight:
            out = out + weight * (1 - 2 * ((index // weight) % 2))
        weight *= 2
    return out


def where01(hit):
    return jnp.where(hit, 1.0, 0.0).astype(BF16)


def iota(shape, dim):
    return lax.broadcasted_iota(jnp.int32, shape, dim)


def dot(a, b):
    return jnp.dot(a, b, preferred_element_type=F32)


def dot_nt(a, b):
    return lax.dot_general(a, b, NT, preferred_element_type=F32)


def kernel(
    peers, capp,
    tok_hbm, gain_hbm, ids_hbm, slots_hbm, wts_hbm, wg_hbm, wu_hbm, wd_hbm,
    out,
    tok, gain, ids, slots, wts, wg, wu, wd,
    earlier, normed, chosen, n_out, n_in, about, spreads, picks, own_picks, homes, home_w,
    x_out, x_in, y_out, e_in, acc, hid, r_out, r_in, m_out, h_in,
    ready, l_sem, w_sem, ns, nr, xs, xr, ys, yr, rs, rr, hs, hr,
):
    rows, feat = tok.shape
    ffn = wg.shape[1]
    block, width = x_out.shape[2:]
    spread = peers * capp
    me = lax.axis_index("ep")
    group, rank = me // peers, me % peers
    inner = (group % 2 + group // 2) % 2
    shift = peers.bit_length() - 1
    mesh_id = pl.DeviceIdType.MESH

    def at(d, j):
        return {"ep": flip(group, d) * peers + flip(rank, j)}

    order = [0, 2 - inner, 1 + inner, 3]

    barrier = pltpu.get_barrier_semaphore()
    for d in range(1, GROUPS):
        @pl.when(flip(group, d) > 0)
        def _():
            pl.semaphore_signal(barrier, inc=1, device_id=at(d, 0), device_id_type=mesh_id)
    for j in range(1, peers):
        pl.semaphore_signal(barrier, inc=1, device_id=at(0, j), device_id_type=mesh_id)

    def fetch(pairs, sem):
        copies = [pltpu.make_async_copy(src, dst, sem.at[i]) for i, (src, dst) in enumerate(pairs)]
        for copy in copies:
            copy.start()
        return copies

    small = fetch(
        ((ids_hbm, ids), (slots_hbm, slots), (wts_hbm, wts), (gain_hbm, gain), (tok_hbm, tok)), l_sem
    )

    def send(src, dst, sent, got, where):
        pltpu.make_async_remote_copy(
            src_ref=src, dst_ref=dst, send_sem=sent, recv_sem=got,
            device_id=where, device_id_type=mesh_id,
        ).start()

    def receive(dst, got):
        pltpu.make_async_remote_copy(
            src_ref=dst, dst_ref=dst, send_sem=xs.at[0], recv_sem=got,
            device_id=at(1, 0), device_id_type=mesh_id,
        ).wait_recv()

    earlier[...] = where01(iota((rows, rows), 0) < iota((rows, rows), 1))
    n_out[...] = jnp.zeros_like(n_out)
    for copy in small[:3]:
        copy.wait()
    tok_group = ids[0:1, :] >> shift
    member = where01(iota((16, rows), 0) == tok_group)
    before = dot(member, earlier[...])
    place = jnp.sum(before * member.astype(F32), axis=0, keepdims=True)
    kind = iota((FACTS, rows), 0)
    facts = jnp.where(kind == 8, tok_group.astype(F32), jnp.where(kind == 9, place, 0.0))
    codes = []
    for k in range(2):
        code = ((ids[k:k + 1, :] & (peers - 1)) ^ rank) * capp + slots[k:k + 1, :] + 1
        codes.append(code)
        facts = jnp.where(kind == k, code.astype(F32), facts)
        w = wts[k:k + 1, :]
        for part in range(3):
            piece = w.astype(BF16).astype(F32)
            facts = jnp.where(kind == 2 + 3 * k + part, piece, facts)
            w = w - piece
    facts = facts.astype(BF16)
    slot = iota((spread, rows), 0) + 1
    chosen[:spread, :] = where01(((slot == codes[0]) | (slot == codes[1])) & (tok_group == group))
    row_no = iota((block, rows), 0).astype(F32)
    for d in range(1, GROUPS):
        mine = where01((row_no == place) & (tok_group == flip(group, d)))
        chosen[spread + (d - 1) * block:spread + d * block, :] = mine

    for copy in small[3:]:
        copy.wait()
    loads = fetch(((wg_hbm, wg), (wu_hbm, wu), (wd_hbm, wd)), w_sem)
    step = 32

    def norm_rows(i, carry):
        at_rows = pl.ds(pl.multiple_of(i * step, step), step)
        v = tok[at_rows, :].astype(F32)
        scale = lax.rsqrt(jnp.mean(v * v, axis=-1, keepdims=True) + 1e-06)
        normed[at_rows, :] = (v * scale * gain[...]).astype(BF16)
        return carry

    lax.fori_loop(0, rows // step, norm_rows, 0, unroll=True)

    far_first = list(range(2, peers)) + [1]
    theirs = pl.ds(capp, spread - capp)

    def send_spread(s, c):
        d = order[s]
        for j in far_first:
            send(y_out.at[d, c, pl.ds((j - 1) * capp, capp)], e_in.at[d, c, pl.ds(j * capp, capp)],
                 ys.at[0], yr.at[d, c], at(0, j))

    def send_back(d, c):
        for j in far_first:
            send(r_out.at[d, c, pl.ds((j - 1) * capp, capp)], r_in.at[d, c, pl.ds(j * capp, capp)],
                 rs.at[0], rr.at[d, c], at(0, j))

    def send_group(d, c):
        send(x_out.at[d - 1, c], x_in.at[d - 1, c], xs.at[0], xr.at[d - 1, c], at(d, 0))

    def enter():
        @pl.when(group == 0)
        def _():
            pl.semaphore_wait(barrier, peers - 1)

        @pl.when(group > 0)
        def _():
            pl.semaphore_wait(barrier, GROUPS - 1 + peers - 1)
        for g in range(1, GROUPS):
            @pl.when(group == g)
            def _():
                pl.semaphore_signal(ready.at[g - 1], inc=1, device_id=at(g, 0), device_id_type=mesh_id)

    def send_facts(d):
        send(n_out.at[d - 1], n_in.at[d - 1], ns.at[0], nr.at[d - 1], at(d, 0))

    for c in range(CHUNKS):
        got = dot(chosen[...], normed[:, c * width:(c + 1) * width]).astype(BF16)
        e_in[0, c, :capp, :] = got[:capp]
        y_out[0, c, :, :] = got[capp:spread]
        for d in range(1, GROUPS):
            x_out[d - 1, c, :, :] = got[spread + (d - 1) * block:spread + d * block]
        if c == 0:
            enter()
        send_spread(0, c)

        @pl.when(group > 0)
        def _():
            send_group(1, c)

        @pl.when(inner == 1)
        def _():
            send_group(2, c)

        if c == 0:
            for d in range(1, GROUPS):
                mine = chosen[spread + (d - 1) * block:spread + d * block, :]
                n_out[d - 1, :, :block] = dot_nt(facts, mine).astype(BF16)

            @pl.when(group > 0)
            def _():
                for d in range(1, GROUPS):
                    send_facts(d)

    @pl.when(group == 0)
    def _():
        pl.semaphore_wait(ready.at[0], 1)
        send_facts(1)
        for c in range(CHUNKS):
            send_group(1, c)

    columns = dot_nt(where01(iota((rows, rows), 0) == iota((rows, rows), 1)), facts)
    slot = (iota((rows, spread), 1) + 1).astype(F32)
    ours = columns[:, 8:9] == group.astype(F32)
    for k in range(2):
        own_picks[k] = where01((slot == columns[:, k:k + 1]) & ours)
        b = 2 + 3 * k
        home_w[k] = columns[:, b:b + 1] + columns[:, b + 1:b + 2] + columns[:, b + 2:b + 3]
    slot = iota((rows, block), 1).astype(F32)
    for d in range(1, GROUPS):
        there = where01((slot == columns[:, 9:10]) & (columns[:, 8:9] == flip(group, d).astype(F32)))
        homes[:, (d - 1) * block:d * block] = there

    def dispatch(s, c):
        d = order[s]
        if c == 0:
            receive(n_in.at[d - 1], nr.at[d - 1])
            info = n_in[d - 1]
            code = info[:, :block].astype(F32)
            slot = (iota((spread, block), 0) + 1).astype(F32)
            spreads[d - 1] = where01((slot == code[0:1, :]) | (slot == code[1:2, :]))
        receive(x_in.at[d - 1, c], xr.at[d - 1, c])
        got = dot(spreads[d - 1], x_in[d - 1, c]).astype(BF16)
        e_in[d, c, :capp, :] = got[:capp]
        y_out[d, c, :, :] = got[capp:]
        send_spread(s, c)
        if c == CHUNKS - 1:
            info = n_in[d - 1]
            facts_of = dot_nt(where01(iota((block, LANES), 0) == iota((block, LANES), 1)), info)
            about[d - 1] = facts_of
            slot = (iota((block, spread), 1) + 1).astype(F32)
            for k in range(2):
                picks[d - 1, k] = where01(slot == facts_of[:, k:k + 1])

    def send_far():
        @pl.when(group == 0)
        def _():
            for d in (2, 3):
                pl.semaphore_wait(ready.at[d - 1], 1)
                send_facts(d)

        @pl.when(inner == 0)
        def _():
            for c in range(CHUNKS):
                send_group(2, c)

        for c in range(CHUNKS):
            send_group(3, c)

    half = min(256, ffn)

    def partial(s, c, w, f):
        return dot(e_in[order[s], c], w[c * width:(c + 1) * width, f])

    def gather(s, c):
        d = order[s]
        if loads:
            for load in loads:
                load.wait()
            loads.clear()
        receive(e_in.at[d, c, theirs], yr.at[d, c])
        if c < CHUNKS - 1:
            for i, w in enumerate((wg, wu)):
                for f in range(0, ffn, half):
                    f = slice(f, f + half)
                    if c == 0:
                        acc[d, i, :, f] = partial(s, c, w, f)
                    else:
                        acc[d, i, :, f] += partial(s, c, w, f)

    def compute(s):
        d, c = order[s], CHUNKS - 1
        gather(s, c)
        for f in range(0, ffn, half):
            f = slice(f, f + half)
            gate = acc[d, 0, :, f] + partial(s, c, wg, f)
            upper = acc[d, 1, :, f] + partial(s, c, wu, f)
            hid[:, f] = (gate / (1.0 + jnp.exp(-gate)) * upper).astype(BF16)
        for c in range(CHUNKS):
            got = dot(hid[...], wd[:, c * width:(c + 1) * width]).astype(BF16)
            r_in[d, c, :capp, :] = got[:capp]
            r_out[d, c, :, :] = got[capp:]
            if s > 1:
                send_back(s, c)

    def mix(d, c, held=False):
        facts_of = about[d - 1]
        weigh = [facts_of[:, b:b + 1] + facts_of[:, b + 1:b + 2] + facts_of[:, b + 2:b + 3] for b in (2, 5)]
        receive(r_in.at[d, c, theirs], rr.at[d, c])
        got = r_in[d, c]
        mixed = weigh[0] * dot(picks[d - 1, 0], got) + weigh[1] * dot(picks[d - 1, 1], got)
        m_out[d - 1, c, :, :] = mixed.astype(BF16)
        if isinstance(d, int) and d == 2 and c < HELD:
            pl.when(inner == 1)(functools.partial(send_home, d, c, flip(group, d)))
        elif isinstance(d, int):
            send_home(d, c, flip(group, d))
        else:
            send_home(d, c, choose(1 - (d - 1) // 2, flip(group, 3), flip(group, 1)))

    def send_home(d, c, there):
        send(m_out.at[d - 1, c], h_in.at[c, d - 1], hs.at[0], hr.at[c], {"ep": there * peers + rank})

    def send_held():
        @pl.when(inner == 0)
        def _():
            for c in range(HELD):
                send_home(2, c, flip(group, 2))

    def choose(which, a, b):
        return a + which * (b - a)

    def last_with(first):
        near = [(1, c) for c in range(CHUNKS)]
        return near[:first] + [(3, c) for c in range(CHUNKS)] + near[first:]

    last, last_inner = last_with(1), last_with(NEAR_FIRST)

    def mix_last(i):
        mix(*(choose(inner, a, b) for a, b in zip(last[i], last_inner[i])))

    def send_back_if(which, d, c):
        pl.when(inner == which)(functools.partial(send_back, d, c))

    def near_back(late):
        @pl.when(inner == 1)
        def _():
            for c in range(NEAR_FIRST, CHUNKS) if late else range(1, NEAR_FIRST):
                send_back(1, c)

        if late:
            @pl.when(inner == 0)
            def _():
                for c in range(1, CHUNKS):
                    send_back(1, c)

    def finish(c):
        receive(h_in.at[c], hr.at[c])
        total = dot(homes[...], h_in[c].reshape(homes.shape[1], width))
        receive(r_in.at[0, c, theirs], rr.at[0, c])
        got = r_in[0, c]
        total += home_w[0] * dot(own_picks[0], got) + home_w[1] * dot(own_picks[1], got)
        out[:, c * width:(c + 1) * width] = total.astype(BF16)

    stages = {"X": send_far, "N": send_held, "D": dispatch, "U": gather, "C": compute, "R": send_back, "M": mix, "L": mix_last, "B": near_back, "Q": send_back_if, "F": finish}
    for item in SCHEDULE:
        stages[item[0]](*(int(i) for i in item[1:]))

    for src, dst, sent, got in (
        (n_out, n_in, ns, nr), (x_out, x_in, xs, xr), (y_out, r_out, ys, yr), (r_out, y_out, rs, rr), (m_out, m_out, hs, hr),
    ):
        pltpu.make_async_remote_copy(
            src_ref=src, dst_ref=dst, send_sem=sent.at[0], recv_sem=got.at[(0,) * len(got.shape)],
            device_id=at(1, 0), device_id_type=mesh_id,
        ).wait_send()


def shards(tokens, norm_gain, route_ids, route_slots, route_weights, w_gate, w_up, w_down):
    rows, feat = tokens.shape
    n_devices = lax.axis_size("ep")
    top_count = route_ids.shape[1]
    cap = 3 * top_count * rows // (2 * n_devices)
    capp = -(-cap // 16) * 16
    peers = n_devices // GROUPS
    block = peers * cap // top_count
    spread = peers * capp
    ffn = w_gate.shape[2]
    width = feat // CHUNKS
    others = GROUPS - 1
    anywhere = pl.BlockSpec(memory_space=pl.ANY)
    vmem = pl.BlockSpec(memory_space=pltpu.VMEM)
    dma = pltpu.SemaphoreType.DMA

    def buf(*shape, kind=BF16):
        return pltpu.VMEM(shape, kind)

    return pl.pallas_call(
        functools.partial(kernel, peers, capp),
        out_shape=pltpu.VMEM((rows, feat), BF16),
        in_specs=[anywhere] * 8,
        out_specs=vmem,
        scratch_shapes=[
            buf(rows, feat), buf(1, feat, kind=F32), buf(top_count, rows, kind=jnp.int32),
            buf(top_count, rows, kind=jnp.int32), buf(top_count, rows, kind=F32),
            buf(feat, ffn), buf(feat, ffn), buf(ffn, feat),
            buf(rows, rows), buf(rows, feat), buf(spread + others * block, rows),
            buf(others, FACTS, LANES), buf(others, FACTS, LANES), buf(others, block, FACTS, kind=F32),
            buf(others, spread, block), buf(others, 2, block, spread), buf(2, rows, spread),
            buf(rows, others * block), buf(2, rows, 1, kind=F32),
            buf(others, CHUNKS, block, width), buf(others, CHUNKS, block, width),
            buf(GROUPS, CHUNKS, spread - capp, width), buf(GROUPS, CHUNKS, spread, width),
            buf(GROUPS, 2, spread, ffn, kind=F32), buf(spread, ffn),
            buf(GROUPS, CHUNKS, spread - capp, width), buf(GROUPS, CHUNKS, spread, width),
            buf(others, CHUNKS, block, width), buf(CHUNKS, others, block, width),
            pltpu.SemaphoreType.REGULAR((GROUPS - 1,)), dma((5,)), dma((3,)),
            dma((1,)), dma((others,)),
            dma((1,)), dma((others, CHUNKS)),
            dma((1,)), dma((GROUPS, CHUNKS)),
            dma((1,)), dma((GROUPS, CHUNKS)),
            dma((1,)), dma((CHUNKS,)),
        ],
        compiler_params=pltpu.CompilerParams(
            collective_id=0, has_side_effects=True, vmem_limit_bytes=60 * 1024 * 1024
        ),
    )(
        tokens, norm_gain.reshape(1, feat), route_ids.T, route_slots.T, route_weights.T,
        w_gate.reshape(feat, ffn), w_up.reshape(feat, ffn), w_down.reshape(ffn, feat),
    )


def solution(mesh):
    placed = (
        P(("grp", "ep"), None),
        P(),
        P(("grp", "ep"), None),
        P(("grp", "ep"), None),
        P(("grp", "ep"), None),
        P("ep", None, None),
        P("ep", None, None),
        P("ep", None, None),
    )
    return jax.shard_map(
        shards, mesh=mesh, in_specs=placed, out_specs=P(("grp", "ep"), None), check_vma=False
    )
```
